32 devices in a mesh: ep: 32 (over z, y, x, core).
Axes of the slice: x: 2, y: 2, z: 4, core: 2. Of those that a mesh axis runs over, the one named last changes fastest.
Arguments:
- tokens: bfloat16 [128, 4, 1024], P('ep'), may hold values from -6 to 6
- lengths: int32 [128], P('ep'), may hold values from 1 to 4, 192 in all
- routes: int32 [128, 4, 8], P('ep'), may hold values from 0 to 63, all different within a row; in each aligned block of 16 rows (0 to 15, 16 to 31, ...) at most 4 rows name the same one
- gates: float32 [128, 4, 8], P('ep'), may hold values from 0.05 to 0.6
- norm_gain: float32 [1024], replicated, may hold values from 0.5 to 1.5
- expert_gate: bfloat16 [64, 1024, 256], P('ep'), may hold values from -0.1875 to 0.1875
- expert_up: bfloat16 [64, 1024, 256], P('ep'), may hold values from -0.1875 to 0.1875
- expert_down: bfloat16 [64, 256, 1024], P('ep'), may hold values from -0.375 to 0.375
- shared_gate: bfloat16 [1024, 256], replicated, may hold values from -0.1875 to 0.1875
- shared_up: bfloat16 [1024, 256], replicated, may hold values from -0.1875 to 0.1875
- shared_down: bfloat16 [256, 1024], replicated, may hold values from -0.375 to 0.375
- out_gain: float32 [1024], replicated, may hold values from 0.5 to 1.5
Outputs:
- mixed: bfloat16 [128, 4, 1024], P('ep')
The draws below stay inside these ranges and needn't reach their ends.
Inputs may be any that keep to these rules, and one draw needn't show every extreme that they name: `routes`: in the 16 rows of one device (all slots, in order), no expert is named by more than 4 rows, and some device reaches 4; the experts of one row differ. `lengths`: each sequence has 1 to 4 live slots, the longest exactly 4.
All inputs are finite; a program needn't handle non-finite values.
Results may differ from the reference program's by a relative error of at most 0.0065.
Values may be sent and summed in bfloat16 or wider, within the bound.
A program may use at most 64 MiB of HBM per device.

```python
import math
import jax
import jax.numpy as jnp
import numpy as np
from jax import lax

D = 1024
FF = 256
SFF = 256
TOP = 8
NEW = 4
MOST = 4
SEQUENCES = 128
TOK_DEV = 16
EXPERTS = 64


def block_scale(rng, shape, split, smallest, high):
    factor_of, own = 1.0, jax.random.fold_in(rng, 6)
    for position, parts in split:
        heights = jnp.exp(jax.random.uniform(jax.random.fold_in(own, position), (parts,), jnp.float32, smallest / len(split), high / len(split)))
        factor_of = factor_of * jnp.repeat(heights, shape[position] // parts).reshape([-1 if axis == position else 1 for axis in range(len(shape))])
    return factor_of


def length_profile(number_of, total, most, skew):
    portions = [(1 << 20) // math.isqrt(rank ** skew) + 1 for rank in range(2, number_of + 1)]
    surplus, given = total - most - (number_of - 1), [1] * (number_of - 1)
    while surplus > 0:
        free = [i for i in range(number_of - 1) if given[i] < most]
        whole, remaining = sum([portions[i] for i in free]), surplus
        for i in free:
            addition = min(most - given[i], max(1, remaining * portions[i] // whole), surplus)
            given[i] = given[i] + addition
            surplus = surplus - addition
    return np.array([most] + given)


def uneven(rng, amount, total, most, lean):
    if amount == 2:
        one = jax.random.randint(rng, (), max(1, total - most), min(most, total - 1) + 1)
        return jnp.stack([one, total - one])
    sizes = jnp.asarray(length_profile(amount, total, most, lean), jnp.int32)
    twos = (amount - 1) // 2
    donor, sink = sizes[1:1 + 2 * twos:2], sizes[2:2 + 2 * twos:2]
    slack = jnp.minimum(donor - 1, most - sink)
    passed = jax.random.randint(jax.random.fold_in(rng, 1), (twos,), 0, 1 << 20) % (slack + 1)
    sizes = sizes.at[1:1 + 2 * twos:2].set(donor - passed).at[2:2 + 2 * twos:2].set(sink + passed)
    return sizes[jax.random.permutation(jax.random.fold_in(rng, 2), amount)]


def shared_out(key, own, number, rows, number_of, top, limit, slope):
    sequence = jax.random.permutation(key, number_of)
    heavy_load, usual = portions_of(number_of, rows * top, limit, slope, True), portions_of(number_of, rows * top, limit, slope, False)
    places = jnp.arange(number_of)

    def named(sizes, rotation):
        used = int((sizes > 0).sum())
        fixed = max(1, used // 4)
        passed = fixed + (places - fixed + rotation * (used - fixed)) % max(1, number_of - fixed)
        return jnp.zeros((number_of,), jnp.int32).at[sequence[jnp.where(places < fixed, places, passed)]].set(jnp.asarray(sizes, jnp.int32))

    sizes = jnp.where(number % 4 == 0, named(heavy_load, number // 4), named(usual, number - number // 4 - 1))
    mixed = jax.random.permutation(jax.random.fold_in(own, 3), number_of)
    donor, sink = mixed[0:number_of // 2 * 2:2], mixed[1:number_of // 2 * 2:2]
    room = jnp.minimum(sizes[donor] - 1, limit - sizes[sink]) // 2
    room = jnp.where((donor == sequence[0]) | (sink == sequence[0]) | (sizes[sink] == 0), 0, jnp.maximum(room, 0))
    passed = jax.random.randint(jax.random.fold_in(own, 4), (number_of // 2,), 0, 1 << 20) % (room + 1)
    sizes = sizes.at[donor].add(-passed).at[sink].add(passed)
    members = jnp.searchsorted(jnp.cumsum(sizes), jnp.arange(rows * top), side="right").astype(jnp.int32)
    grid = members.reshape(top, rows).T
    grid = grid[jax.random.permutation(jax.random.fold_in(own, 1), rows)]
    rotation = jax.random.randint(jax.random.fold_in(own, 2), (rows, 1), 0, top)
    return jnp.take_along_axis(grid, (jnp.arange(top)[None, :] + rotation) % top, axis=1)


def portions_of(number_of, total, limit, lean, full):
    portions = [(1 << 20) // math.isqrt(standing ** lean) + 1 for standing in range(1, number_of + 1)]
    largest = limit if full else min(limit, max(-(-total // number_of), total * portions[0] // sum(portions)))
    least = 1 if total - largest >= number_of - 1 else 0
    holding, rest = [largest] + [least] * (number_of - 1), total - largest - least * (number_of - 1)
    while rest > 0:
        free = [i for i in range(1, number_of) if holding[i] < largest] or [i for i in range(1, number_of) if holding[i] < limit]
        whole, budget = sum([portions[i] for i in free]), rest
        for i in free:
            addition = min(limit - holding[i], max(1, budget * portions[i] // whole), rest)
            holding[i] = holding[i] + addition
            rest = rest - addition
    return np.array(holding)


def centred(own_key, shape, spread, bound, shards=(), kind=jnp.bfloat16):
    entries = jax.random.normal(own_key, shape, jnp.float32) * spread
    if len(shards) > 0:
        entries = block_scale(own_key, shape, shards, -0.22, 0.18) * entries
    return jnp.clip(entries, min=-bound, max=bound).astype(kind)


def setup_inputs(seed: int = 0) -> dict:
    streams_of = jax.random.split(jax.random.key(seed), 13)
    tokens = centred(streams_of[0], (SEQUENCES, NEW, D), 1.0, 6.0, ((0, 32),))
    lengths = uneven(streams_of[1], SEQUENCES, SEQUENCES * 3 // 2, NEW, 2).astype(jnp.int32)
    routes_keys = jax.random.split(jax.random.fold_in(streams_of[2], 1), SEQUENCES * NEW // TOK_DEV)
    routes_turns = jax.random.permutation(jax.random.fold_in(streams_of[2], 3), SEQUENCES * NEW // TOK_DEV)
    routes = jax.vmap(lambda own, number: shared_out(jax.random.fold_in(streams_of[2], 2), own, number, TOK_DEV, EXPERTS, TOP, MOST, 2))(routes_keys, routes_turns).reshape((SEQUENCES, NEW, TOP))
    gates = jnp.clip(0.05 + 0.55 * jax.random.uniform(streams_of[3], (SEQUENCES, NEW, TOP), jnp.float32) ** block_scale(streams_of[3], (SEQUENCES, NEW, TOP), ((0, 32),), -0.2, 0.2), 0.05, 0.6)
    norm_gain = jnp.clip(1.0 + 0.1 * jax.random.normal(streams_of[4], (D,), jnp.float32), 0.5, 1.5)
    expert_gate = centred(streams_of[5], (EXPERTS, D, FF), D ** -0.5, 0.1875, ((0, 32),))
    expert_up = centred(streams_of[6], (EXPERTS, D, FF), D ** -0.5, 0.1875, ((0, 32),))
    expert_down = centred(streams_of[7], (EXPERTS, FF, D), FF ** -0.5, 0.375, ((0, 32),))
    shared_gate = centred(streams_of[8], (D, SFF), D ** -0.5, 0.1875)
    shared_up = centred(streams_of[9], (D, SFF), D ** -0.5, 0.1875)
    shared_down = centred(streams_of[10], (SFF, D), SFF ** -0.5, 0.375)
    out_gain = jnp.clip(1.0 + 0.1 * jax.random.normal(streams_of[11], (D,), jnp.float32), 0.5, 1.5)
    return {"tokens": tokens, "lengths": lengths, "routes": routes, "gates": gates, "norm_gain": norm_gain, "expert_gate": expert_gate, "expert_up": expert_up, "expert_down": expert_down, "shared_gate": shared_gate, "shared_up": shared_up, "shared_down": shared_down, "out_gain": out_gain}


EPS = 1e-06

def norm_rows(values, scales):
    wide = values.astype(jnp.float32)
    return wide * lax.rsqrt(lax.optimization_barrier(jnp.mean(wide * wide, axis=-1, keepdims=True)) + EPS) * scales

def reference(tokens, lengths, routes, gates, norm_gain, expert_gate, expert_up, expert_down, shared_gate, shared_up, shared_down, out_gain):
    features = tokens.shape[-1]
    flat_rows = tokens.reshape(-1, features)
    normed = norm_rows(flat_rows, norm_gain).astype(jnp.bfloat16)
    live_mask = (jnp.arange(NEW, dtype=jnp.int32)[None, :] < lengths[:, None]).reshape(-1)
    expert_ids = routes.reshape(-1)
    copies = jnp.repeat(normed, TOP, axis=0)
    block_rows = 32
    row_blocks = copies.reshape(-1, block_rows, features)
    id_blocks = expert_ids.reshape(-1, block_rows)

    def one_block(pair):
        rows_in, ids_in = pair
        wide_rows = rows_in.astype(jnp.float32)
        gate_part = jnp.einsum('rd,rdf->rf', wide_rows, expert_gate[ids_in].astype(jnp.float32))
        up_part = jnp.einsum('rd,rdf->rf', wide_rows, expert_up[ids_in].astype(jnp.float32))
        hidden = (jax.nn.silu(gate_part) * up_part).astype(jnp.bfloat16)
        result = jnp.einsum('rf,rfd->rd', hidden.astype(jnp.float32), expert_down[ids_in].astype(jnp.float32))
        return result.astype(jnp.bfloat16)
    outputs = lax.map(one_block, (row_blocks, id_blocks)).reshape(-1, TOP, features)
    weights = jnp.where(live_mask[:, None], gates.reshape(-1, TOP), jnp.float32(0.0))
    routed = lax.optimization_barrier(jnp.sum(weights[:, :, None] * outputs.astype(jnp.float32), axis=1))
    shared_hidden = (jax.nn.silu(jnp.dot(normed, shared_gate, preferred_element_type=jnp.float32)) * jnp.dot(normed, shared_up, preferred_element_type=jnp.float32)).astype(jnp.bfloat16)
    shared = jnp.dot(shared_hidden, shared_down, preferred_element_type=jnp.float32)
    summed = routed + shared
    mixed_out = jnp.where(live_mask[:, None], norm_rows(summed, out_gain), jnp.float32(0.0))
    return mixed_out.astype(jnp.bfloat16).reshape(tokens.shape)
```

```python
import functools
import jax
import jax.numpy as jnp
from jax import lax
from jax.experimental import pallas as pl
from jax.experimental.pallas import tpu as pltpu
from jax.sharding import PartitionSpec as P

EPS = 1e-06
META = 128
PLANE = 4
CORES = 2
MESH = pl.DeviceIdType.MESH
ANY = pl.ANY


def silu(v):
    return v / (1.0 + jnp.exp(-v))


def layer_kernel(
    line,
    tokens_ref, lengths_ref, routes_ref, gates_ref, norm_ref,
    eg_hbm, eu_hbm, ed_hbm, sg_hbm, su_hbm, sd_hbm, outgain_ref,
    out_ref,
    rows_scr, meta_scr, got, wg, wu, wd, sg, su, sd, acts, part, got_a, got_b, got_c, shared_scr,
    w_sem, w_send, w_recv, g_recv, z_send, x_send, y_send, d_send,
    a_send, a_recv, b_send, b_recv, c_send, c_recv,
):
    me = lax.axis_index("ep")
    core = lax.rem(me, CORES)
    x_bit = lax.rem(me // CORES, 2)
    y_bit = lax.rem(me // (CORES * 2), 2)
    group = CORES * PLANE
    z = me // group
    low = lax.rem(me, group)
    partner = me + 1 - 2 * core
    x_peer = me + CORES * (1 - 2 * x_bit)
    y_peer = me + 2 * CORES * (1 - 2 * y_bit)

    def z_peer(step):
        return lax.rem(z + step + line, line) * group + low

    seqs, new, feats = tokens_ref.shape
    rows = seqs * new
    top = routes_ref.shape[2]
    local = eg_hbm.shape[0]
    half = line // 2

    barrier = pltpu.get_barrier_semaphore()
    peers = [partner, x_peer, y_peer] + [z_peer(r) for r in range(1, line)]
    for peer in peers:
        pl.semaphore_signal(barrier, inc=1, device_id=(peer,), device_id_type=MESH)

    mine = pl.ds(core * local, local)
    loads = []
    for i, (src, dst) in enumerate(((eg_hbm, wg), (eu_hbm, wu), (ed_hbm, wd))):
        loads.append(pltpu.make_async_copy(src, dst.at[mine], w_sem.at[i]))
    for i, (src, dst) in enumerate(((sg_hbm, sg), (su_hbm, su), (sd_hbm, sd))):
        loads.append(pltpu.make_async_copy(src, dst, w_sem.at[3 + i]))
    for load in loads:
        load.start()

    steps = lax.broadcasted_iota(jnp.int32, (new, top), 0)
    meta_scr[...] = jnp.zeros_like(meta_scr)
    for s in range(seqs):
        at = pl.ds(s * new, new)
        rows_scr[at, :] = tokens_ref[s].astype(jnp.float32)
        live = steps < lengths_ref[s]
        gate = jnp.where(live, gates_ref[s], 0.0)
        high = gate.astype(jnp.bfloat16).astype(jnp.float32)
        meta_scr[at, 0:top] = routes_ref[s].astype(jnp.float32)
        meta_scr[at, top:2 * top] = high
        meta_scr[at, 2 * top:3 * top] = gate - high
    wide = rows_scr[...]
    scale = lax.rsqrt(jnp.mean(wide * wide, axis=-1, keepdims=True) + EPS)
    normed = (wide * scale * norm_ref[...]).astype(jnp.bfloat16)
    got[0, 0, :, 0:feats] = normed
    got[0, 0, :, feats:feats + META] = meta_scr[...].astype(jnp.bfloat16)

    pl.semaphore_wait(barrier, len(peers))

    def send(src, dst, ssem, rsem, peer):
        return pltpu.make_async_remote_copy(
            src_ref=src, dst_ref=dst, send_sem=ssem, recv_sem=rsem,
            device_id=(peer,), device_id_type=MESH,
        )

    z_copy = {
        r: send(got.at[0, 0], got.at[0, r], z_send.at[r], g_recv.at[0, r], z_peer(-r))
        for r in range(1, line)
    }
    x_copy = [send(got.at[0, r], got.at[1, r], x_send.at[r], g_recv.at[1, r], x_peer) for r in range(line)]
    y_copy = [send(got.at[0, r], got.at[2, r], y_send.at[r], g_recv.at[2, r], y_peer) for r in range(line)]
    d_copy = [
        send(got.at[1, r], got.at[3, r], d_send.at[r], g_recv.at[3, r], y_peer)
        if r < half
        else send(got.at[2, r], got.at[3, r], d_send.at[r], g_recv.at[3, r], x_peer)
        for r in range(line)
    ]
    order = sorted(range(line), key=lambda r: (min(r, line - r), r))
    for r in order[1:]:
        z_copy[r].start()
    x_copy[0].start()
    y_copy[0].start()
    w_copy = [
        send(src, dst.at[mine], w_send.at[i], w_recv.at[i], partner)
        for i, (src, dst) in enumerate(((eg_hbm, wg), (eu_hbm, wu), (ed_hbm, wd)))
    ]
    for copy in w_copy:
        copy.start()

    for load in loads[3:]:
        load.wait()
    own = got[0, 0, :, 0:feats]
    s_hidden = (
        silu(jnp.dot(own, sg[...], preferred_element_type=jnp.float32))
        * jnp.dot(own, su[...], preferred_element_type=jnp.float32)
    ).astype(jnp.bfloat16)
    shared_scr[...] = jnp.dot(s_hidden, sd[...], preferred_element_type=jnp.float32)

    def relay(r):
        if r < half:
            x_copy[r].wait_recv()
        else:
            y_copy[r].wait_recv()
        d_copy[r].start()

    for i, r in enumerate(order[1:]):
        z_copy[r].wait_recv()
        x_copy[r].start()
        y_copy[r].start()
        relay(order[i])
    relay(order[-1])
    for r in range(line):
        if r < half:
            y_copy[r].wait_recv()
        else:
            x_copy[r].wait_recv()
    for load in loads[:3]:
        load.wait()
    for copy in w_copy:
        copy.wait_recv()

    experts = local * CORES
    hidden_size = wg.shape[2]
    first = (me // CORES) * experts

    def compute(rels):
        lo, count = rels[0], len(rels)
        m = count * line * rows
        stacked = got[lo:lo + count, :, :, 0:feats].reshape(m, feats)
        meta = got[lo:lo + count, :, :, feats:feats + META].reshape(m, META).astype(jnp.float32)
        ids = meta[:, 0:top]
        gate = meta[:, top:2 * top] + meta[:, 2 * top:3 * top]
        for e in range(experts):
            named = (first + e).astype(jnp.float32)
            weight = jnp.sum(jnp.where(ids == named, gate, 0.0), axis=1, keepdims=True)
            gate_part = jnp.dot(stacked, wg[e], preferred_element_type=jnp.float32)
            up_part = jnp.dot(stacked, wu[e], preferred_element_type=jnp.float32)
            acts[0:m, e * hidden_size:(e + 1) * hidden_size] = (
                silu(gate_part) * up_part * weight
            ).astype(jnp.bfloat16)
        tile = 256
        for c in range(0, feats, tile):
            down = wd[:, :, c:c + tile].reshape(experts * hidden_size, tile)
            outs = jnp.dot(acts[0:m, :], down, preferred_element_type=jnp.float32)
            part[lo:lo + count, :, :, c:c + tile] = outs.reshape(count, line, rows, tile).astype(jnp.bfloat16)

    a_copy = [
        send(part.at[3, r], got_a.at[r], a_send.at[r], a_recv.at[r], x_peer if r < half else y_peer)
        for r in range(line)
    ]
    b_copy = [
        [send(part.at[1 + i, r], got_b.at[i, r], b_send.at[i, r], b_recv.at[i, r], peer) for r in range(line)]
        for i, peer in enumerate((x_peer, y_peer))
    ]
    c_copy = {
        r: send(part.at[0, r], got_c.at[r], c_send.at[r], c_recv.at[r], z_peer(r))
        for r in range(1, line)
    }

    compute((0, 1, 2))
    for r in range(line):
        b_copy[0 if r < half else 1][r].start()
    for r in range(line):
        d_copy[r].wait_recv()
    compute((3,))
    for r in order:
        a_copy[r].start()
    for r in order:
        a_copy[r].wait_recv()
        i = 1 if r < half else 0
        part[1 + i, r] = (
            part[1 + i, r].astype(jnp.float32) + got_a[r].astype(jnp.float32)
        ).astype(jnp.bfloat16)
        b_copy[i][r].start()

    def column(r):
        b_copy[0][r].wait_recv()
        b_copy[1][r].wait_recv()
        return (
            part[0, r].astype(jnp.float32)
            + got_b[0, r].astype(jnp.float32)
            + got_b[1, r].astype(jnp.float32)
        )

    for r in order[1:]:
        part[0, r] = column(r).astype(jnp.bfloat16)
        c_copy[r].start()
    summed = column(0) + shared_scr[...]
    for r in order[1:]:
        c_copy[r].wait_recv()
        summed = summed + got_c[r].astype(jnp.float32)
    scale = lax.rsqrt(jnp.mean(summed * summed, axis=-1, keepdims=True) + EPS)
    rows_scr[...] = summed * scale * outgain_ref[...]
    steps = lax.broadcasted_iota(jnp.int32, (new, feats), 0)
    for s in range(seqs):
        live = steps < lengths_ref[s]
        out_ref[s] = jnp.where(live, rows_scr[pl.ds(s * new, new), :], 0.0).astype(out_ref.dtype)

    for copies in (w_copy, x_copy, y_copy, d_copy, a_copy, b_copy[0], b_copy[1],
                   list(z_copy.values()), list(c_copy.values())):
        for copy in copies:
            copy.wait_send()


def per_device(
    tokens, lengths, routes, gates, norm_gain,
    expert_gate, expert_up, expert_down, shared_gate, shared_up, shared_down, out_gain,
):
    devices = lax.axis_size("ep")
    line = devices // (CORES * PLANE)
    seqs, new, feats = tokens.shape
    rows = seqs * new
    local, _, hidden = expert_gate.shape
    experts = local * CORES
    bf, f32 = jnp.bfloat16, jnp.float32
    vm = pl.BlockSpec(memory_space=pltpu.VMEM)
    hbm = pl.BlockSpec(memory_space=ANY)
    dma = pltpu.SemaphoreType.DMA
    return pl.pallas_call(
        functools.partial(layer_kernel, line),
        out_shape=jax.ShapeDtypeStruct(tokens.shape, tokens.dtype),
        in_specs=[vm, pl.BlockSpec(memory_space=pltpu.SMEM), vm, vm, vm] + [hbm] * 6 + [vm],
        out_specs=vm,
        scratch_shapes=[
            pltpu.VMEM((rows, feats), f32),
            pltpu.VMEM((rows, META), f32),
            pltpu.VMEM((PLANE, line, rows, feats + META), bf),
            pltpu.VMEM((experts, feats, hidden), bf),
            pltpu.VMEM((experts, feats, hidden), bf),
            pltpu.VMEM((experts, hidden, feats), bf),
            pltpu.VMEM(shared_gate.shape, bf),
            pltpu.VMEM(shared_up.shape, bf),
            pltpu.VMEM(shared_down.shape, bf),
            pltpu.VMEM(((PLANE - 1) * line * rows, experts * hidden), bf),
            pltpu.VMEM((PLANE, line, rows, feats), bf),
            pltpu.VMEM((line, rows, feats), bf),
            pltpu.VMEM((2, line, rows, feats), bf),
            pltpu.VMEM((line, rows, feats), bf),
            pltpu.VMEM((rows, feats), f32),
            dma((6,)), dma((3,)), dma((3,)),
            dma((PLANE, line)), dma((line,)), dma((line,)), dma((line,)), dma((line,)),
            dma((line,)), dma((line,)), dma((2, line)), dma((2, line)), dma((line,)), dma((line,)),
        ],
        compiler_params=pltpu.CompilerParams(collective_id=0, has_side_effects=True),
    )(
        tokens, lengths, routes, gates, norm_gain.reshape(1, feats),
        expert_gate, expert_up, expert_down, shared_gate, shared_up, shared_down,
        out_gain.reshape(1, feats),
    )


def solution(mesh):
    split = P("ep", None, None)
    placed = (split, P("ep"), split, split, P(), split, split, split, P(), P(), P(), P())
    return jax.shard_map(
        per_device, mesh=mesh, in_specs=placed, out_specs=split, check_vma=False
    )
```

```python
import functools
import jax
import jax.numpy as jnp
from jax import lax
from jax.experimental import pallas as pl
from jax.experimental.pallas import tpu as pltpu
from jax.sharding import PartitionSpec as P

EPS = 1e-06
META = 128
PLANE = 4
CORES = 2
MESH = pl.DeviceIdType.MESH
ANY = pl.ANY


def silu(v):
    return v / (1.0 + jnp.exp(-v))


def layer_kernel(
    line,
    tokens_ref, lengths_ref, routes_ref, gates_ref, norm_ref,
    eg_hbm, eu_hbm, ed_hbm, sg_hbm, su_hbm, sd_hbm, outgain_ref,
    out_ref,
    rows_scr, meta_scr, got, wg, wu, wd, sg, su, sd, acts, part, got_a, got_b, got_c, shared_scr,
    w_sem, w_send, w_recv, g_recv, z_send, x_send, y_send, d_send,
    a_send, a_recv, b_send, b_recv, c_send, c_recv,
):
    me = lax.axis_index("ep")
    core = lax.rem(me, CORES)
    x_bit = lax.rem(me // CORES, 2)
    y_bit = lax.rem(me // (CORES * 2), 2)
    group = CORES * PLANE
    z = me // group
    low = lax.rem(me, group)
    partner = me + 1 - 2 * core
    x_peer = me + CORES * (1 - 2 * x_bit)
    y_peer = me + 2 * CORES * (1 - 2 * y_bit)
    xy_peer = x_peer + y_peer - me

    def z_peer(step):
        return lax.rem(z + step + line, line) * group + low

    seqs, new, feats = tokens_ref.shape
    rows = seqs * new
    top = routes_ref.shape[2]
    local = eg_hbm.shape[0]
    half = line // 2

    barrier = pltpu.get_barrier_semaphore()
    peers = [partner, x_peer, y_peer, xy_peer] + [z_peer(r) for r in range(1, line)]
    for peer in peers:
        pl.semaphore_signal(barrier, inc=1, device_id=(peer,), device_id_type=MESH)

    mine = pl.ds(core * local, local)
    loads = []
    for i, (src, dst) in enumerate(((eg_hbm, wg), (eu_hbm, wu), (ed_hbm, wd))):
        loads.append(pltpu.make_async_copy(src, dst.at[mine], w_sem.at[i]))
    for i, (src, dst) in enumerate(((sg_hbm, sg), (su_hbm, su), (sd_hbm, sd))):
        loads.append(pltpu.make_async_copy(src, dst, w_sem.at[3 + i]))
    for load in loads:
        load.start()

    steps = lax.broadcasted_iota(jnp.int32, (new, top), 0)
    meta_scr[...] = jnp.zeros_like(meta_scr)
    for s in range(seqs):
        at = pl.ds(s * new, new)
        rows_scr[at, :] = tokens_ref[s].astype(jnp.float32)
        live = steps < lengths_ref[s]
        gate = jnp.where(live, gates_ref[s], 0.0)
        high = gate.astype(jnp.bfloat16).astype(jnp.float32)
        meta_scr[at, 0:top] = routes_ref[s].astype(jnp.float32)
        meta_scr[at, top:2 * top] = high
        meta_scr[at, 2 * top:3 * top] = gate - high
    wide = rows_scr[...]
    scale = lax.rsqrt(jnp.mean(wide * wide, axis=-1, keepdims=True) + EPS)
    normed = (wide * scale * norm_ref[...]).astype(jnp.bfloat16)
    got[0, 0, :, 0:feats] = normed
    got[0, 0, :, feats:feats + META] = meta_scr[...].astype(jnp.bfloat16)

    pl.semaphore_wait(barrier, len(peers))

    def send(src, dst, ssem, rsem, peer):
        return pltpu.make_async_remote_copy(
            src_ref=src, dst_ref=dst, send_sem=ssem, recv_sem=rsem,
            device_id=(peer,), device_id_type=MESH,
        )

    z_copy = {
        r: send(got.at[0, 0], got.at[0, r], z_send.at[r], g_recv.at[0, r], z_peer(-r))
        for r in range(1, line)
    }
    x_copy = [send(got.at[0, r], got.at[1, r], x_send.at[r], g_recv.at[1, r], x_peer) for r in range(line)]
    y_copy = [send(got.at[0, r], got.at[2, r], y_send.at[r], g_recv.at[2, r], y_peer) for r in range(line)]
    d_copy = [send(got.at[0, r], got.at[3, r], d_send.at[r], g_recv.at[3, r], xy_peer) for r in range(line)]
    order = sorted(range(line), key=lambda r: (min(r, line - r), r))
    for r in order[1:]:
        z_copy[r].start()
    x_copy[0].start()
    y_copy[0].start()
    d_copy[0].start()
    w_copy = [
        send(src, dst.at[mine], w_send.at[i], w_recv.at[i], partner)
        for i, (src, dst) in enumerate(((eg_hbm, wg), (eu_hbm, wu), (ed_hbm, wd)))
    ]
    for copy in w_copy:
        copy.start()

    for r in order[1:]:
        z_copy[r].wait_recv()
        x_copy[r].start()
        y_copy[r].start()
        d_copy[r].start()
    for r in order:
        x_copy[r].wait_recv()
        y_copy[r].wait_recv()
    for load in loads[:3]:
        load.wait()
    for copy in w_copy:
        copy.wait_recv()

    experts = local * CORES
    hidden_size = wg.shape[2]
    first = (me // CORES) * experts

    def compute(rels):
        lo, count = rels[0], len(rels)
        m = count * line * rows
        stacked = got[lo:lo + count, :, :, 0:feats].reshape(m, feats)
        meta = got[lo:lo + count, :, :, feats:feats + META].reshape(m, META).astype(jnp.float32)
        ids = meta[:, 0:top]
        gate = meta[:, top:2 * top] + meta[:, 2 * top:3 * top]
        for e in range(experts):
            named = (first + e).astype(jnp.float32)
            weight = jnp.sum(jnp.where(ids == named, gate, 0.0), axis=1, keepdims=True)
            gate_part = jnp.dot(stacked, wg[e], preferred_element_type=jnp.float32)
            up_part = jnp.dot(stacked, wu[e], preferred_element_type=jnp.float32)
            acts[0:m, e * hidden_size:(e + 1) * hidden_size] = (
                silu(gate_part) * up_part * weight
            ).astype(jnp.bfloat16)
        tile = 256
        for c in range(0, feats, tile):
            down = wd[:, :, c:c + tile].reshape(experts * hidden_size, tile)
            outs = jnp.dot(acts[0:m, :], down, preferred_element_type=jnp.float32)
            part[lo:lo + count, :, :, c:c + tile] = outs.reshape(count, line, rows, tile).astype(jnp.bfloat16)

    a_copy = [send(part.at[3, r], got_a.at[r], a_send.at[r], a_recv.at[r], xy_peer) for r in range(line)]
    b_copy = [
        [send(part.at[1 + i, r], got_b.at[i, r], b_send.at[i, r], b_recv.at[i, r], peer) for r in range(line)]
        for i, peer in enumerate((x_peer, y_peer))
    ]
    c_copy = {
        r: send(part.at[0, r], got_c.at[r], c_send.at[r], c_recv.at[r], z_peer(r))
        for r in range(1, line)
    }

    compute((0, 1, 2))
    for r in range(line):
        d_copy[r].wait_recv()
    compute((3,))
    far = order[::-1]
    for r in far:
        a_copy[r].start()
    for r in far:
        b_copy[0][r].start()
        b_copy[1][r].start()

    for load in loads[3:]:
        load.wait()
    own = got[0, 0, :, 0:feats]
    s_hidden = (
        silu(jnp.dot(own, sg[...], preferred_element_type=jnp.float32))
        * jnp.dot(own, su[...], preferred_element_type=jnp.float32)
    ).astype(jnp.bfloat16)
    shared_scr[...] = jnp.dot(s_hidden, sd[...], preferred_element_type=jnp.float32)

    def column(r):
        b_copy[0][r].wait_recv()
        b_copy[1][r].wait_recv()
        a_copy[r].wait_recv()
        return (
            part[0, r].astype(jnp.float32)
            + got_b[0, r].astype(jnp.float32)
            + got_b[1, r].astype(jnp.float32)
            + got_a[r].astype(jnp.float32)
        )

    for r in far[:-1]:
        part[0, r] = column(r).astype(jnp.bfloat16)
        c_copy[r].start()
    summed = column(0) + shared_scr[...]
    for r in far[:-1]:
        c_copy[r].wait_recv()
        summed = summed + got_c[r].astype(jnp.float32)
    scale = lax.rsqrt(jnp.mean(summed * summed, axis=-1, keepdims=True) + EPS)
    mixed = summed * scale * outgain_ref[...]
    steps = lax.broadcasted_iota(jnp.int32, (rows, feats), 0)
    for s in range(seqs):
        dead = (steps >= s * new + lengths_ref[s]) & (steps < (s + 1) * new)
        mixed = jnp.where(dead, 0.0, mixed)
    out_ref[...] = mixed.astype(out_ref.dtype)

    for copies in (w_copy, x_copy, y_copy, d_copy, a_copy, b_copy[0], b_copy[1],
                   list(z_copy.values()), list(c_copy.values())):
        for copy in copies:
            copy.wait_send()


def per_device(
    tokens, lengths, routes, gates, norm_gain,
    expert_gate, expert_up, expert_down, shared_gate, shared_up, shared_down, out_gain,
):
    devices = lax.axis_size("ep")
    line = devices // (CORES * PLANE)
    seqs, new, feats = tokens.shape
    rows = seqs * new
    local, _, hidden = expert_gate.shape
    experts = local * CORES
    bf, f32 = jnp.bfloat16, jnp.float32
    vm = pl.BlockSpec(memory_space=pltpu.VMEM)
    hbm = pl.BlockSpec(memory_space=ANY)
    dma = pltpu.SemaphoreType.DMA
    return pl.pallas_call(
        functools.partial(layer_kernel, line),
        out_shape=jax.ShapeDtypeStruct((rows, feats), tokens.dtype),
        in_specs=[vm, pl.BlockSpec(memory_space=pltpu.SMEM), vm, vm, vm] + [hbm] * 6 + [vm],
        out_specs=vm,
        scratch_shapes=[
            pltpu.VMEM((rows, feats), f32),
            pltpu.VMEM((rows, META), f32),
            pltpu.VMEM((PLANE, line, rows, feats + META), bf),
            pltpu.VMEM((experts, feats, hidden), bf),
            pltpu.VMEM((experts, feats, hidden), bf),
            pltpu.VMEM((experts, hidden, feats), bf),
            pltpu.VMEM(shared_gate.shape, bf),
            pltpu.VMEM(shared_up.shape, bf),
            pltpu.VMEM(shared_down.shape, bf),
            pltpu.VMEM(((PLANE - 1) * line * rows, experts * hidden), bf),
            pltpu.VMEM((PLANE, line, rows, feats), bf),
            pltpu.VMEM((line, rows, feats), bf),
            pltpu.VMEM((2, line, rows, feats), bf),
            pltpu.VMEM((line, rows, feats), bf),
            pltpu.VMEM((rows, feats), f32),
            dma((6,)), dma((3,)), dma((3,)),
            dma((PLANE, line)), dma((line,)), dma((line,)), dma((line,)), dma((line,)),
            dma((line,)), dma((line,)), dma((2, line)), dma((2, line)), dma((line,)), dma((line,)),
        ],
        compiler_params=pltpu.CompilerParams(collective_id=0, has_side_effects=True),
    )(
        tokens, lengths, routes, gates, norm_gain.reshape(1, feats),
        expert_gate, expert_up, expert_down, shared_gate, shared_up, shared_down,
        out_gain.reshape(1, feats),
    ).reshape(tokens.shape)


def solution(mesh):
    split = P("ep", None, None)
    placed = (split, P("ep"), split, split, P(), split, split, split, P(), P(), P(), P())
    return jax.shard_map(
        per_device, mesh=mesh, in_specs=placed, out_specs=split, check_vma=False
    )
```
